32 devices in a mesh: grp: 2 (over y), ep: 16 (over z, x, core), tp: 1.
Axes of the slice: x: 2, y: 2, z: 4, core: 2. Of those that a mesh axis runs over, the one named last changes fastest.
Arguments:
- tokens: bfloat16 [2048, 2048], P(('grp', 'ep')), parts along dimension 0, may hold values from -6 to 6
- norm_gain: float32 [2048], replicated, may hold values from 0.1 to 1.9
- routes: int32 [2048, 6], P(('grp', 'ep')), parts along dimension 0, may hold values from 0 to 15, all different within a row; in each aligned block of 64 rows (0 to 63, 64 to 127, ...) at most 48 rows name the same one
- gates: float32 [2048, 6], P(('grp', 'ep')), parts along dimension 0, may hold values from 0.2 to 1
- expert_gate: bfloat16 [16, 2048, 512], P('ep', None, 'tp'), may hold values from -0.125 to 0.125
- expert_up: bfloat16 [16, 2048, 512], P('ep', None, 'tp'), may hold values from -0.125 to 0.125
- expert_down: bfloat16 [16, 512, 2048], P('ep', 'tp'), may hold values from -0.25 to 0.25
- shared_gate: bfloat16 [2048, 512], P(None, 'tp'), may hold values from -0.125 to 0.125
- shared_up: bfloat16 [2048, 512], P(None, 'tp'), may hold values from -0.125 to 0.125
- shared_down: bfloat16 [512, 2048], P('tp'), may hold values from -0.25 to 0.25
Outputs:
- mixed: bfloat16 [2048, 2048], P(('grp', 'ep'), 'tp'), parts along dimension 0
The draws below stay inside these ranges and needn't reach their ends.
There are 2 independent parts, one for each index of `grp`. The reference program is written for one: setup_inputs(seed, part) draws one part's arguments, and reference() takes and returns one part's arrays. A program takes and returns all parts, laid end to end along the dimension named above; an argument that names none is the same for every part. Nothing has to cross between parts.
Inputs may be any that keep to these rules, and one draw needn't show every extreme that they name: `routes`: each row names 6 different experts. In the rows of one index of ep no expert is named by more than 48 rows, and in some such block an expert is named by exactly 48 rows.
All inputs are finite; a program needn't handle non-finite values.
Results may differ from the reference program's by a relative error of at most 0.01.
Values may be sent and summed in bfloat16 or wider, within the bound.
No kernel may reach another device: no remote copies, remote signals or barrier semaphores. Data moves between devices by JAX's collectives and lax.ppermute only.
A program may use at most 64 MiB of HBM per device.

```python
import math
import jax
import jax.numpy as jnp
import numpy as np
from jax import lax

D = 2048
FF = 512
SFF = 512
TOP_K = 6
TOK_DEV = 64
EXPERTS = 16
TOKENS = 1024
CAP = 48
N_EP = 16
N_TP = 1


def shard_levels(rng, shape, shards, low, top_value):
    def one(axis_at, parts):
        steps = jax.random.uniform(jax.random.fold_in(jax.random.fold_in(rng, 6), axis_at), (parts,), jnp.float32, low / len(shards), top_value / len(shards))
        return jnp.repeat(jnp.exp(steps), shape[axis_at] // parts).reshape((-1,) + (1,) * (len(shape) - axis_at - 1))

    gain = one(*shards[0])
    for cut in shards[1:]:
        gain = gain * one(*cut)
    return gain


def assign_block(stream_key, own, number, rows, amount, top, most, slope):
    order = jax.random.permutation(stream_key, amount)
    heavy_load, usual = shares(amount, rows * top, most, slope, True), shares(amount, rows * top, most, slope, False)
    places = jnp.arange(amount)

    def named(sizes, rotation):
        used = int((sizes > 0).sum())
        fixed = max(1, used // 4)
        shifted = fixed + (places - fixed + rotation * (used - fixed)) % max(1, amount - fixed)
        return jnp.zeros((amount,), jnp.int32).at[order[jnp.where(places < fixed, places, shifted)]].set(jnp.asarray(sizes, jnp.int32))

    sizes = jnp.where(number % 4 == 0, named(heavy_load, number // 4), named(usual, number - number // 4 - 1))
    mixed = jax.random.permutation(jax.random.fold_in(own, 3), amount)
    giver, receiver = mixed[0:amount // 2 * 2:2], mixed[1:amount // 2 * 2:2]
    room = jnp.minimum(sizes[giver] - 1, most - sizes[receiver]) // 2
    room = jnp.where((giver == order[0]) | (receiver == order[0]) | (sizes[receiver] == 0), 0, jnp.maximum(room, 0))
    shifted = jax.random.randint(jax.random.fold_in(own, 4), (amount // 2,), 0, 1 << 20) % (room + 1)
    sizes = sizes.at[giver].add(-shifted).at[receiver].add(shifted)
    members = jnp.searchsorted(jnp.cumsum(sizes), jnp.arange(rows * top), side="right").astype(jnp.int32)
    grid = members.reshape(top, rows).T
    grid = grid[jax.random.permutation(jax.random.fold_in(own, 1), rows)]
    rotation = jax.random.randint(jax.random.fold_in(own, 2), (rows, 1), 0, top)
    return jnp.take_along_axis(grid, (jnp.arange(top)[None, :] + rotation) % top, axis=1)


def shares(amount, total, most, slope, full):
    portions = [(1 << 20) // math.isqrt(standing ** slope) + 1 for standing in range(1, amount + 1)]
    largest = most if full else min(most, max(-(-total // amount), total * portions[0] // sum(portions)))
    least = 1 if total - largest >= amount - 1 else 0
    holding, surplus = [largest] + [least] * (amount - 1), total - largest - least * (amount - 1)
    while surplus > 0:
        candidates = [i for i in range(1, amount) if holding[i] < largest] or [i for i in range(1, amount) if holding[i] < most]
        whole, remaining = sum([portions[i] for i in candidates]), surplus
        for i in candidates:
            extra = min(most - holding[i], max(1, remaining * portions[i] // whole), surplus)
            holding[i] = holding[i] + extra
            surplus = surplus - extra
    return np.array(holding)


def centred(own_key, dims, scale, reach, cuts=(), held_as=jnp.bfloat16):
    array = scale * jax.random.normal(own_key, dims, jnp.float32)
    if cuts:
        array = array * shard_levels(own_key, dims, cuts, -0.22, 0.18)
    return jnp.clip(array, -reach, reach).astype(held_as)


def setup_inputs(seed: int = 0, part: int = 0) -> dict:
    arg_keys = jax.random.split(jax.random.key(seed), 11)
    part_keys = jax.random.split(jax.random.fold_in(arg_keys[10], part), 11)
    tokens = centred(part_keys[0], (TOKENS, D), 1.0, 6.0, ((0, 16),))
    norm_gain = jnp.clip(1.0 + 0.18 * jax.random.normal(arg_keys[1], (D,), jnp.float32), 0.1, 1.9)
    routes_keys = jax.random.split(jax.random.fold_in(part_keys[2], 1), TOKENS // TOK_DEV)
    routes_turns = jax.random.permutation(jax.random.fold_in(part_keys[2], 3), TOKENS // TOK_DEV)
    routes = jax.vmap(lambda own, number: assign_block(jax.random.fold_in(part_keys[2], 2), own, number, TOK_DEV, EXPERTS, TOP_K, CAP, 2))(routes_keys, routes_turns).reshape((TOKENS, TOP_K))
    gates = jnp.clip(jnp.exp(math.log(1.0) - 1.609438 * jax.random.uniform(part_keys[3], (TOKENS, TOP_K), jnp.float32) ** shard_levels(part_keys[3], (TOKENS, TOP_K), ((0, 16),), -0.2, 0.2)), 0.2, 1.0)
    expert_gate = centred(arg_keys[4], (EXPERTS, D, FF), D ** -0.5, 0.125, ((0, 16),))
    expert_up = centred(arg_keys[5], (EXPERTS, D, FF), D ** -0.5, 0.125, ((0, 16),))
    expert_down = centred(arg_keys[6], (EXPERTS, FF, D), FF ** -0.5, 0.25, ((0, 16),))
    shared_gate = centred(arg_keys[7], (D, SFF), D ** -0.5, 0.125)
    shared_up = centred(arg_keys[8], (D, SFF), D ** -0.5, 0.125)
    shared_down = centred(arg_keys[9], (SFF, D), SFF ** -0.5, 0.25)
    return dict(tokens=tokens, norm_gain=norm_gain, routes=routes, gates=gates, expert_gate=expert_gate, expert_up=expert_up, expert_down=expert_down, shared_gate=shared_gate, shared_up=shared_up, shared_down=shared_down)


def reference(tokens, norm_gain, routes, gates, expert_gate, expert_up, expert_down, shared_gate, shared_up, shared_down):
    values = tokens.astype(jnp.float32)
    scale = lax.rsqrt(lax.optimization_barrier(jnp.mean(values * values, axis=1, keepdims=True)) + 1e-06)
    normed = (values * scale * norm_gain[None, :]).astype(jnp.bfloat16)
    shared_hidden = (jax.nn.silu(jnp.dot(normed, shared_gate, preferred_element_type=jnp.float32)) * jnp.dot(normed, shared_up, preferred_element_type=jnp.float32)).astype(jnp.bfloat16)
    shared_out = jnp.dot(shared_hidden, shared_down, preferred_element_type=jnp.float32)
    bound = N_EP * CAP

    def one_expert(expert, total):
        chosen = routes == expert
        weight = lax.optimization_barrier(jnp.sum(jnp.where(chosen, gates, jnp.float32(0.0)), axis=1))
        live = jnp.any(chosen, axis=1).astype(jnp.int32)
        order = jnp.argsort(1 - live, stable=True)[:bound].astype(jnp.int32)
        rows = normed[order]
        hidden = (jax.nn.silu(jnp.dot(rows, expert_gate[expert], preferred_element_type=jnp.float32)) * jnp.dot(rows, expert_up[expert], preferred_element_type=jnp.float32)).astype(jnp.bfloat16)
        halves = hidden.reshape(bound, N_TP, FF // N_TP).astype(jnp.float32)
        down = expert_down[expert].reshape(N_TP, FF // N_TP, D).astype(jnp.float32)
        partial_value = jnp.einsum('rtf,tfd->trd', halves, down).astype(jnp.bfloat16).astype(jnp.float32)
        result = lax.optimization_barrier(jnp.sum(partial_value, axis=0))
        return total.at[order].add(weight[order][:, None] * result)
    routed = lax.fori_loop(0, EXPERTS, one_expert, jnp.zeros((TOKENS, D), jnp.float32))
    return (routed + shared_out).astype(jnp.bfloat16)
```

```python
import jax
import jax.numpy as jnp
from jax import lax
from jax.sharding import PartitionSpec as P

LANES = 128


def split_ranks(ranks):
    core = 2 if ranks % 2 == 0 else 1
    near = 2 if (ranks // core) % 2 == 0 else 1
    return ranks // (core * near), near, core


def permute(rows, ranks, move):
    far, near, core = split_ranks(ranks)
    pairs = []
    for z in range(far):
        for a in range(near):
            for c in range(core):
                z_to, a_to, c_to = move(z, a, c)
                pairs.append(((z * near + a) * core + c, (z_to * near + a_to) * core + c_to))
    return lax.ppermute(rows, "ep", pairs)


def hop(z, step, far):
    return z ^ step if far & (far - 1) == 0 else (z + step) % far


def hop_back(z, step, far):
    return z ^ step if far & (far - 1) == 0 else (z - step) % far


def dot(a, b):
    return jnp.dot(a, b, preferred_element_type=jnp.float32)


def gated(rows, w_gate, w_up):
    return (jax.nn.silu(dot(rows, w_gate)) * dot(rows, w_up)).astype(jnp.bfloat16)


def add(a, b):
    return (a.astype(jnp.float32) + b.astype(jnp.float32)).astype(jnp.bfloat16)


def shards(
    tokens,
    norm_gain,
    routes,
    gates,
    expert_gate,
    expert_up,
    expert_down,
    shared_gate,
    shared_up,
    shared_down,
):
    count, width = tokens.shape
    local_experts = expert_gate.shape[0]
    ranks = lax.axis_size("ep")
    all_experts = local_experts * ranks
    far, near, core = split_ranks(ranks)
    values = tokens.astype(jnp.float32)
    scale = lax.rsqrt(jnp.mean(values * values, axis=1, keepdims=True) + 1e-06)
    normed = (values * scale * norm_gain[None, :]).astype(jnp.bfloat16)

    chosen = routes[:, :, None] == jnp.arange(all_experts, dtype=jnp.int32)[None, None, :]
    weight = jnp.sum(jnp.where(chosen, gates[:, :, None], 0.0), axis=1)
    high = lax.reduce_precision(weight, 8, 7)
    middle = lax.reduce_precision(weight - high, 8, 7)
    low = weight - high - middle
    pieces = jnp.concatenate([high, middle, low], axis=1).astype(jnp.bfloat16)
    pad = -pieces.shape[1] % LANES
    own = jnp.concatenate([normed, jnp.pad(pieces, ((0, 0), (0, pad)))], axis=1)

    first = lax.axis_index("ep") * local_experts

    def experts(rows):
        data = rows[:, :width]
        parts = rows[:, width:].astype(jnp.float32)
        column = jnp.arange(parts.shape[1], dtype=jnp.int32)
        total = None
        for e in range(local_experts):
            mine = (column % all_experts == first + e) & (column < 3 * all_experts)
            w = jnp.sum(jnp.where(mine[None, :], parts, 0.0), axis=1, keepdims=True)
            out = w * dot(gated(data, expert_gate[e], expert_up[e]), expert_down[e])
            total = out if total is None else total + out
        return total.astype(jnp.bfloat16)

    arrived = [own] + [
        permute(own, ranks, lambda z, a, c, s=s: (hop(z, s, far), a, c)) for s in range(1, far)
    ]
    back = [None] * far
    for s in list(range(1, far)) + [0]:
        lane = arrived[s]
        if near == 2:
            other = permute(lane, ranks, lambda z, a, c: (z, 1 - a, c))
            lane = jnp.concatenate([lane, other], axis=0)
        block = lane
        if core == 2:
            other = permute(lane, ranks, lambda z, a, c: (z, a, 1 - c))
            block = jnp.concatenate([lane, other], axis=0)
        result = experts(block)
        half = lane.shape[0]
        if core == 2:
            other = permute(result[half:], ranks, lambda z, a, c: (z, a, 1 - c))
            result = add(result[:half], other)
        if near == 2:
            other = permute(result[count:], ranks, lambda z, a, c: (z, 1 - a, c))
            result = add(result[:count], other)
        if s:
            result = permute(result, ranks, lambda z, a, c, s=s: (hop_back(z, s, far), a, c))
        back[s] = result

    shared_out = dot(gated(normed, shared_gate, shared_up), shared_down)
    routed = sum(part.astype(jnp.float32) for part in back)
    payload = routed + shared_out
    return lax.psum_scatter(payload.astype(jnp.bfloat16), "tp", scatter_dimension=1, tiled=True)


def solution(mesh):
    in_specs = (
        P(("grp", "ep"), None),
        P(),
        P(("grp", "ep"), None),
        P(("grp", "ep"), None),
        P("ep", None, "tp"),
        P("ep", None, "tp"),
        P("ep", "tp", None),
        P(None, "tp"),
        P(None, "tp"),
        P("tp", None),
    )
    out_specs = P(("grp", "ep"), "tp")
    return jax.shard_map(shards, mesh=mesh, in_specs=in_specs, out_specs=out_specs, check_vma=False)
```

```python
import jax
import jax.numpy as jnp
from jax import lax
from jax.sharding import PartitionSpec as P


LANES = 128


def split_ranks(ranks):
    core = 2 if ranks % 2 == 0 else 1
    near = 2 if (ranks // core) % 2 == 0 else 1
    return ranks // (core * near), near, core


def permute_rows(rows, ranks, move):
    far, near, core = split_ranks(ranks)
    pairs = []
    for z in range(far):
        for a in range(near):
            for c in range(core):
                z_to, a_to, c_to = move(z, a, c)
                pairs.append(((z * near + a) * core + c, (z_to * near + a_to) * core + c_to))
    return lax.ppermute(rows, "ep", pairs)


def hop(z, step, far):
    return z ^ step if far & (far - 1) == 0 else (z + step) % far


def hop_back(z, step, far):
    return z ^ step if far & (far - 1) == 0 else (z - step) % far


def dot(a, b):
    return jnp.dot(a, b, preferred_element_type=jnp.float32)


def gated(rows, w_gate, w_up):
    return (jax.nn.silu(dot(rows, w_gate)) * dot(rows, w_up)).astype(jnp.bfloat16)


def add(a, b):
    return (a.astype(jnp.float32) + b.astype(jnp.float32)).astype(jnp.bfloat16)


def shards(
    tokens,
    norm_gain,
    routes,
    gates,
    expert_gate,
    expert_up,
    expert_down,
    shared_gate,
    shared_up,
    shared_down,
):
    count, width = tokens.shape
    local_experts = expert_gate.shape[0]
    ranks = lax.axis_size("ep")
    all_experts = local_experts * ranks
    far, near, core = split_ranks(ranks)
    values = tokens.astype(jnp.float32)
    scale = lax.rsqrt(jnp.mean(values * values, axis=1, keepdims=True) + 1e-06)
    normed = (values * scale * norm_gain[None, :]).astype(jnp.bfloat16)

    chosen = routes[:, :, None] == jnp.arange(all_experts, dtype=jnp.int32)[None, None, :]
    weight = jnp.sum(jnp.where(chosen, gates[:, :, None], 0.0), axis=1)
    high = lax.reduce_precision(weight, 8, 7)
    middle = lax.reduce_precision(weight - high, 8, 7)
    low = weight - high - middle
    pieces = jnp.concatenate([high, middle, low], axis=1).astype(jnp.bfloat16)
    pad = -pieces.shape[1] % LANES
    own = jnp.concatenate([normed, jnp.pad(pieces, ((0, 0), (0, pad)))], axis=1)

    first = lax.axis_index("ep") * local_experts

    def weights(rows, e):
        parts = rows[:, width:].astype(jnp.float32)
        column = jnp.arange(parts.shape[1], dtype=jnp.int32)
        mine = (column % all_experts == first + e) & (column < 3 * all_experts)
        return jnp.sum(jnp.where(mine[None, :], parts, 0.0), axis=1, keepdims=True)

    def experts(rows, cuts):
        totals = [None] * (len(cuts) - 1)
        for e in range(local_experts):
            hidden = gated(rows[:, :width], expert_gate[e], expert_up[e])
            scales = weights(rows, e)
            for i in range(len(totals)):
                part = slice(cuts[i], cuts[i + 1])
                out = scales[part] * dot(hidden[part], expert_down[e])
                totals[i] = out if totals[i] is None else totals[i] + out
        return [total.astype(jnp.bfloat16) for total in totals]

    visits = order(far)
    arrived = {0: own}
    for s in visits:
        arrived[s] = permute_rows(own, ranks, lambda z, a, c, s=s: (hop(z, s, far), a, c))
    lanes = {}
    for s in [0] + visits:
        lanes[s] = arrived[s]
        if near == 2:
            other = permute_rows(lanes[s], ranks, lambda z, a, c: (z, 1 - a, c))
            lanes[s] = jnp.concatenate([lanes[s], other], axis=0)
    shared_out = dot(gated(normed, shared_gate, shared_up), shared_down)
    back = {}
    before = None
    for s in [0] + visits:
        lane = lanes[s]
        half = lane.shape[0]
        if core == 2:
            other = permute_rows(lane, ranks, lambda z, a, c: (z, a, 1 - c))
            block = jnp.concatenate([other, lane], axis=0)
            if before is not None:
                block, before = lax.optimization_barrier((block, before))
            theirs, result = experts(block, (0, half, 2 * half))
            before = theirs
            other = permute_rows(before, ranks, lambda z, a, c: (z, a, 1 - c))
            if near == 2:
                theirs = add(result[count:], other[count:])
                result = add(result[:count], other[:count])
            else:
                result = add(result, other)
        else:
            if near == 2:
                result, theirs = experts(lane, (0, count, half))
            else:
                (result,) = experts(lane, (0, half))
        if near == 2:
            other = permute_rows(theirs, ranks, lambda z, a, c: (z, 1 - a, c))
            result = add(result, other)
        if s:
            result = permute_rows(result, ranks, lambda z, a, c, s=s: (hop_back(z, s, far), a, c))
        back[s] = result

    payload = shared_out
    for s in [0] + visits:
        payload = payload + back[s].astype(jnp.float32)
    return lax.psum_scatter(payload.astype(jnp.bfloat16), "tp", scatter_dimension=1, tiled=True)


def order(far):
    return [3, 2, 1] if far == 4 else list(range(1, far))


def solution(mesh):
    in_specs = (
        P(("grp", "ep"), None),
        P(),
        P(("grp", "ep"), None),
        P(("grp", "ep"), None),
        P("ep", None, "tp"),
        P("ep", None, "tp"),
        P("ep", "tp", None),
        P(None, "tp"),
        P(None, "tp"),
        P("tp", None),
    )
    out_specs = P(("grp", "ep"), "tp")

    return jax.shard_map(shards, mesh=mesh, in_specs=in_specs, out_specs=out_specs, check_vma=False)
```
